1024 devices in a mesh: rep: 16 (over z), fs: 8 (over y), tp: 8 (over x, core).
Axes of the slice: x: 4, y: 8, z: 16, core: 2. Of those that a mesh axis runs over, the one named last changes fastest.
Arguments:
- layer_input: bfloat16 [12288, 2048], P('rep', ('fs', 'tp')), may hold values from -0.56640625 to 0.56640625
- gate_saved: bfloat16 [12288, 5120], P('rep', 'tp'), may hold values from -6 to 6
- up_saved: bfloat16 [12288, 5120], P('rep', 'tp'), may hold values from -6 to 6
- out_grad: bfloat16 [12288, 2048], P('rep'), may hold values from -0.56640625 to 0.56640625
- conv_taps: bfloat16 [3, 5120], P(None, 'tp'), may hold values from -3.5 to 3.5
- w_gate: bfloat16 [2048, 5120], P('fs', 'tp'), may hold values from -0.125 to 0.125
- w_up: bfloat16 [2048, 5120], P('fs', 'tp'), may hold values from -0.125 to 0.125
- w_down: bfloat16 [5120, 2048], P('tp', 'fs'), may hold values from -0.078125 to 0.078125
Outputs:
- input_grad: bfloat16 [12288, 2048], P('rep', ('fs', 'tp'))
- gate_grad: float32 [2048, 5120], P('fs', 'tp')
- up_grad: float32 [2048, 5120], P('fs', 'tp')
- down_grad: float32 [5120, 2048], P('tp', 'fs')
- taps_grad: float32 [3, 5120], P(None, 'tp')
The draws below stay inside these ranges and needn't reach their ends.
All inputs are finite; a program needn't handle non-finite values.
Results may differ from the reference program's by a relative error of at most 0.018.
Values may be sent and summed in bfloat16 or wider, within the bound.
No kernel may reach another device: no remote copies, remote signals or barrier semaphores. Data moves between devices by JAX's collectives and lax.ppermute only.
A program may use at most 64 MiB of HBM per device.

```python
import jax
import jax.numpy as jnp
from jax import lax

D = 2048
FF = 5120
TAPS = 3
TOK_DEV = 768
TOKENS = 12288
HID_TP = 640
N_TP = 8


def spiked(array, stream_key, source, target, shards_of, factor):
    def block_of(position):
        return (jnp.arange(array.shape[position]) // (array.shape[position] // shards_of)).reshape((-1,) + (1,) * (array.ndim - 1 - position))

    one_side = jax.random.permutation(stream_key, shards_of)[block_of(target)]
    second = (block_of(target) + shards_of // 2) % shards_of
    return jnp.where((block_of(source) == one_side) | (block_of(source) == second), factor * array, array)


def level_of(key, shape, cuts, smallest, largest):
    loudness = 1.0
    for dim, shards_of in cuts:
        steps = jax.random.uniform(jax.random.fold_in(jax.random.fold_in(key, 6), dim), (shards_of,), jnp.float32, smallest / len(cuts), largest / len(cuts))
        loudness = loudness * jnp.repeat(jnp.exp(steps), shape[dim] // shards_of).reshape((-1,) + (1,) * (len(shape) - 1 - dim))
    return loudness


def bell_draw(own_key, dims, width, most, cuts=(), held_as=jnp.bfloat16):
    level = level_of(own_key, dims, cuts, -0.22, 0.18) if cuts else 1.0
    values = jax.random.normal(own_key, dims, jnp.float32) * width * level
    return jnp.minimum(jnp.maximum(values, -most), most).astype(held_as)


def heavy_noise(key, shape, scale, bound, split, heavy, dtype=jnp.bfloat16):
    drawn = scale * jax.random.normal(key, shape, jnp.float32)
    if split:
        drawn = drawn * level_of(key, shape, split, -0.22, 0.18)
    return jnp.clip(spiked(drawn, jax.random.fold_in(key, 3), *heavy), -bound, bound).astype(dtype)


def setup_inputs(seed: int = 0) -> dict:
    key_list = jax.random.split(jax.random.key(seed), 9)
    layer_input = bell_draw(key_list[0], (TOKENS, D), (TOKENS ** -0.25), 0.56640625, ((0, 16), (1, 64)))
    gate_saved = bell_draw(key_list[1], (TOKENS, FF), 1.0, 6.0, ((0, 16), (1, 8)))
    up_saved = bell_draw(key_list[2], (TOKENS, FF), 1.0, 6.0, ((0, 16), (1, 8)))
    out_grad = heavy_noise(key_list[3], (TOKENS, D), (TOKENS ** -0.25), 0.56640625, ((0, 16),), (0, 1, 16, 2.0))
    conv_taps = bell_draw(key_list[4], (TAPS, FF), TAPS ** -0.5, 3.5, ((1, 8),))
    w_gate = bell_draw(key_list[5], (D, FF), D ** -0.5, 0.125, ((0, 8), (1, 8)))
    w_up = bell_draw(key_list[6], (D, FF), D ** -0.5, 0.125, ((0, 8), (1, 8)))
    w_down = bell_draw(key_list[7], (FF, D), FF ** -0.5, 0.078125, ((0, 8), (1, 8)))
    return {"layer_input": layer_input, "gate_saved": gate_saved, "up_saved": up_saved, "out_grad": out_grad, "conv_taps": conv_taps, "w_gate": w_gate, "w_up": w_up, "w_down": w_down}


def shift_back(values, count):
    padded = jnp.pad(values, ((0, 0), (count, 0), (0, 0)))
    return padded[:, :TOK_DEV]


def shift_ahead(values, count):
    padded = jnp.pad(values, ((0, 0), (0, count), (0, 0)))
    return padded[:, count:]


def reference(layer_input, gate_saved, up_saved, out_grad, conv_taps, w_gate, w_up, w_down):
    act_grad = jnp.dot(out_grad, w_down.T, preferred_element_type=jnp.float32)
    seq_count = TOKENS // TOK_DEV
    gate_float = gate_saved.astype(jnp.float32).reshape(seq_count, TOK_DEV, FF)
    up_float = up_saved.astype(jnp.float32).reshape(seq_count, TOK_DEV, FF)
    grad_float = act_grad.reshape(seq_count, TOK_DEV, FF)
    taps_float = conv_taps.astype(jnp.float32)
    back_one = shift_back(gate_float, 1)
    back_two = shift_back(gate_float, 2)
    conv_out = taps_float[0] * back_two + taps_float[1] * back_one + taps_float[2] * gate_float
    gate_sig = jax.nn.sigmoid(conv_out)
    swish_out = conv_out * gate_sig
    activation = (swish_out * up_float).astype(jnp.bfloat16).reshape(TOKENS, FF)
    up_part = (grad_float * swish_out).astype(jnp.bfloat16).reshape(TOKENS, FF)
    conv_grad = grad_float * up_float * gate_sig * (1.0 + conv_out * (1.0 - gate_sig))
    ahead_one = shift_ahead(conv_grad, 1)
    ahead_two = shift_ahead(conv_grad, 2)
    gate_part = (taps_float[0] * ahead_two + taps_float[1] * ahead_one + taps_float[2] * conv_grad)
    gate_part = gate_part.astype(jnp.bfloat16).reshape(TOKENS, FF)
    taps_grad = jnp.stack([jnp.sum(conv_grad * back_two, axis=(0, 1)),
                           jnp.sum(conv_grad * back_one, axis=(0, 1)),
                           jnp.sum(conv_grad * gate_float, axis=(0, 1))])
    down_grad = jnp.dot(activation.T, out_grad, preferred_element_type=jnp.float32)
    gate_grad = jnp.dot(layer_input.T, gate_part, preferred_element_type=jnp.float32)
    up_grad = jnp.dot(layer_input.T, up_part, preferred_element_type=jnp.float32)
    gate_blocks = gate_part.astype(jnp.float32).reshape(TOKENS, N_TP, HID_TP)
    up_blocks = up_part.astype(jnp.float32).reshape(TOKENS, N_TP, HID_TP)
    wgate_blocks = w_gate.astype(jnp.float32).reshape(D, N_TP, HID_TP)
    wup_blocks = w_up.astype(jnp.float32).reshape(D, N_TP, HID_TP)
    block_term = jnp.einsum('thf,dhf->htd', gate_blocks, wgate_blocks) + jnp.einsum('thf,dhf->htd', up_blocks, wup_blocks)
    block_term = lax.optimization_barrier(block_term.astype(jnp.bfloat16))
    input_grad = jnp.sum(block_term.astype(jnp.float32), axis=0).astype(jnp.bfloat16)
    return (input_grad, gate_grad, up_grad, down_grad, taps_grad)
```

```python
import jax
import jax.numpy as jnp
from jax import lax
from jax.experimental import pallas as pl
from jax.experimental.pallas import tpu as pltpu
from jax.sharding import PartitionSpec as P

LANES = 128
ROWS = 8
DOWN_ROWS = 32
TAPS = 3


def product(left, right, dims):
    return lax.dot_general(left, right, (dims, ((), ())), preferred_element_type=jnp.float32)


def moved(values, count):
    tokens = values.shape[0]
    row = lax.broadcasted_iota(jnp.int32, values.shape, 0)
    inside = (row >= count) if count > 0 else (row < tokens + count)
    return jnp.where(inside, pltpu.roll(values, count % tokens, 0), 0.0)


def lanes_of(c):
    return pl.ds(pl.multiple_of(c * LANES, LANES), LANES)


def split_rows(out, values):
    rows = out[0].shape[0]
    for i, ref in enumerate(out):
        ref[...] = values[i * rows : (i + 1) * rows]


def slabs(length, rows, width):
    return [pltpu.VMEM((rows, width), jnp.bfloat16)] * (length // rows)


def whole(array):
    return pl.BlockSpec(array.shape, lambda c, *_: (0,) * len(array.shape))


def conv_kernel(place, gate, up, taps, grad, down, swish_out, slope_out, *refs):
    down_out, act_out = refs[: LANES // DOWN_ROWS], refs[LANES // DOWN_ROWS :]
    share = product(grad[...], down[...], ((1,), (1,))).astype(jnp.bfloat16)
    for i, ref in enumerate(act_out):
        ref[:, lanes_of(pl.program_id(0))] = share[i * ROWS : (i + 1) * ROWS]
    gate_float = gate[...].astype(jnp.float32)
    up_float = up[...].astype(jnp.float32)
    taps_float = taps[...].astype(jnp.float32)
    conv_out = (
        taps_float[0:1] * moved(gate_float, 2)
        + taps_float[1:2] * moved(gate_float, 1)
        + taps_float[2:3] * gate_float
    )
    sig = jax.nn.sigmoid(conv_out)
    swish = conv_out * sig
    swish_out[...] = swish.astype(jnp.bfloat16)
    slope_out[...] = (up_float * sig * (1.0 + conv_out * (1.0 - sig))).astype(jnp.bfloat16)
    activation = (swish * up_float).astype(jnp.bfloat16)
    split_rows(down_out, product(activation, grad[...], ((0,), (0,))).astype(jnp.bfloat16))


def conv_cells(place, gate_saved, up_saved, conv_taps, out_grad, w_down):
    tokens, hidden = gate_saved.shape
    block = w_down.shape[1]
    acts = slabs(tokens, ROWS, hidden)
    columns = pl.BlockSpec((tokens, LANES), lambda c, s: (0, c))
    cells = pltpu.HBM((tokens, hidden), jnp.bfloat16)
    run = LANES // DOWN_ROWS
    down = pltpu.HBM((hidden // run, block), jnp.bfloat16)
    return pl.pallas_call(
        conv_kernel,
        out_shape=[cells, cells] + [down] * run + acts,
        grid_spec=pltpu.PrefetchScalarGridSpec(
            num_scalar_prefetch=1,
            grid=(hidden // LANES,),
            in_specs=[
                columns,
                columns,
                pl.BlockSpec((TAPS, LANES), lambda c, s: (0, c)),
                pl.BlockSpec((tokens, block), lambda c, s: (0, s[0])),
                pl.BlockSpec((LANES, block), lambda c, s: (c, 0)),
            ],
            out_specs=[columns, columns]
            + [pl.BlockSpec((DOWN_ROWS, block), lambda c, s: (c, 0))] * run
            + [whole(a) for a in acts],
        ),
        compiler_params=pltpu.CompilerParams(vmem_limit_bytes=16 << 20),
        name="conv_cells",
    )(place, gate_saved, up_saved, conv_taps, out_grad, w_down)


def taken(refs, counts):
    runs = []
    for count in counts:
        runs.append(refs[:count])
        refs = refs[count:]
    return *runs, refs


def grad_kernel(counts, taps, swish, slope, gate, inputs, w_gate, w_up, *refs):
    acts, downs, (terms_out, taps_out), gate_out, up_out, down_out, (terms,) = taken(refs, counts)
    c = pl.program_id(0)
    for i, down in enumerate(downs):
        for j in range(len(down_out) // len(downs)):

            @pl.when(c == j)
            def copy(ref=down_out[j * len(downs) + i], down=down):
                ref[...] = down[...]

    act_grad = jnp.concatenate([a[:, lanes_of(c)] for a in acts], 0).astype(jnp.float32)
    up_part = (act_grad * swish[...].astype(jnp.float32)).astype(jnp.bfloat16)
    conv_grad = act_grad * slope[...].astype(jnp.float32)
    taps_float = taps[...].astype(jnp.float32)
    ahead_one, ahead_two = moved(conv_grad, -1), moved(conv_grad, -2)
    gate_part = (
        taps_float[0:1] * ahead_two + taps_float[1:2] * ahead_one + taps_float[2:3] * conv_grad
    ).astype(jnp.bfloat16)
    gate_float = gate[...].astype(jnp.float32)
    sums = [
        jnp.sum(ahead * gate_float, axis=0, keepdims=True)
        for ahead in (ahead_two, ahead_one, conv_grad)
    ]
    taps_out[:, lanes_of(c)] = jnp.concatenate(sums, 0).astype(jnp.bfloat16)
    for out, part in ((gate_out, gate_part), (up_out, up_part)):
        grads = product(inputs[...], part, ((1,), (0,))).astype(jnp.bfloat16)
        for i, ref in enumerate(out):
            ref[:, lanes_of(c)] = grads[i * ROWS : (i + 1) * ROWS]
    term = product(w_gate[...], gate_part, ((1,), (1,))) + product(w_up[...], up_part, ((1,), (1,)))

    @pl.when(c == 0)
    def first():
        terms[...] = term

    @pl.when(c > 0)
    def later():
        terms[...] += term

    @pl.when(c == pl.num_programs(0) - 1)
    def last():
        terms_out[...] = terms[...].astype(jnp.bfloat16)


def grad_cells(conv_taps, swish, slope, gate_saved, inputs, w_gate, w_up, acts, downs):
    tokens, hidden = swish.shape
    block = inputs.shape[0]
    columns = pl.BlockSpec((tokens, LANES), lambda c: (0, c))
    weights = pl.BlockSpec((block, LANES), lambda c: (0, c))
    grads = slabs(block, ROWS, hidden)
    kept = slabs(hidden, DOWN_ROWS, block)
    out = [
        pltpu.HBM((block, tokens), jnp.bfloat16),
        pltpu.VMEM((TAPS, hidden), jnp.bfloat16),
    ] + grads * 2 + kept
    counts = [len(acts), len(downs), 2, len(grads), len(grads), len(kept)]
    return pl.pallas_call(
        lambda *refs: grad_kernel(counts, *refs),
        out_shape=out,
        grid=(hidden // LANES,),
        in_specs=[pl.BlockSpec((TAPS, LANES), lambda c: (0, c)), columns, columns, columns]
        + [whole(inputs), weights, weights]
        + [whole(a) for a in acts]
        + [pl.BlockSpec((DOWN_ROWS, block), lambda c: (c, 0))] * len(downs),
        out_specs=[whole(o) for o in out],
        scratch_shapes=[pltpu.VMEM((block, tokens), jnp.float32)],
        compiler_params=pltpu.CompilerParams(vmem_limit_bytes=24 << 20),
        name="grad_cells",
    )(conv_taps, swish, slope, gate_saved, inputs, w_gate, w_up, *acts, *downs)


def widen_kernel(counts, *refs):
    ins, outs = refs[: sum(counts)], refs[sum(counts) :]
    for out, count in zip(outs, counts):
        rows = out.shape[0] // count
        for i, ref in enumerate(ins[:count]):
            out[i * rows : (i + 1) * rows, :] = ref[...].astype(jnp.float32)
        ins = ins[count:]


def widened(groups):
    out = [
        jax.ShapeDtypeStruct((sum(a.shape[0] for a in g), g[0].shape[1]), jnp.float32)
        for g in groups
    ]
    return pl.pallas_call(
        lambda *refs: widen_kernel([len(g) for g in groups], *refs),
        out_shape=out,
        compiler_params=pltpu.CompilerParams(vmem_limit_bytes=16 << 20),
        name="widened",
    )(*[a for g in groups for a in g])


def local(layer_input, gate_saved, up_saved, out_grad, conv_taps, w_gate, w_up, w_down):
    gate_saved, up_saved, out_grad, w_gate, w_up, w_down = [
        pltpu.with_memory_space_constraint(a, pltpu.HBM)
        for a in (gate_saved, up_saved, out_grad, w_gate, w_up, w_down)
    ]
    tp = lax.axis_size("tp")
    tokens = out_grad.shape[0]
    block = w_gate.shape[0]
    place = lax.axis_index("fs").astype(jnp.int32).reshape(1)
    inputs = jnp.broadcast_to(layer_input.T[None], (tp, block // tp, tokens))
    inputs = lax.all_to_all(inputs, "tp", 0, 0, tiled=True).reshape(block, tokens)
    run = LANES // DOWN_ROWS
    swish, slope, *rest = conv_cells(place, gate_saved, up_saved, conv_taps, out_grad, w_down)
    downs, acts = rest[:run], rest[run:]
    acts = [pltpu.with_memory_space_constraint(a, pltpu.VMEM) for a in lax.psum(acts, "fs")]
    inputs, swish, slope, *downs = [
        pltpu.with_memory_space_constraint(a, pltpu.HBM) for a in (inputs, swish, slope, *downs)
    ]
    terms, taps, *grads = grad_cells(
        conv_taps, swish, slope, gate_saved, inputs, w_gate, w_up, acts, downs
    )
    terms = lax.all_to_all(terms.reshape(tp, block // tp, tokens), "tp", 0, 0, tiled=True)
    input_grad = jnp.sum(terms.astype(jnp.float32), axis=0).astype(jnp.bfloat16).T
    *grads, taps = [
        pltpu.with_memory_space_constraint(a, pltpu.VMEM) for a in lax.psum([*grads, taps], "rep")
    ]
    half = block // ROWS
    groups = [grads[:half], grads[half : 2 * half], grads[2 * half :], [taps]]
    gate_grad, up_grad, down_grad, taps_grad = widened(groups)
    return (input_grad, gate_grad, up_grad, down_grad, taps_grad)


def solution(mesh):
    placed = (
        P("rep", ("fs", "tp")),
        P("rep", "tp"),
        P("rep", "tp"),
        P("rep", None),
        P(None, "tp"),
        P("fs", "tp"),
        P("fs", "tp"),
        P("tp", "fs"),
    )
    return jax.shard_map(
        local,
        mesh=mesh,
        in_specs=placed,
        out_specs=(
            P("rep", ("fs", "tp")),
            P("fs", "tp"),
            P("fs", "tp"),
            P("tp", "fs"),
            P(None, "tp"),
        ),
        check_vma=False,
    )
```

```python
import jax
import jax.numpy as jnp
from jax import lax
from jax.experimental import pallas as pl
from jax.experimental.pallas import tpu as pltpu
from jax.sharding import PartitionSpec as P

LANES = 128
ROWS = 48
DOWN_ROWS = 64
TAPS = 3


def product(left, right, dims):
    return lax.dot_general(left, right, (dims, ((), ())), preferred_element_type=jnp.float32)


def moved(values, count):
    tokens = values.shape[0]
    row = lax.broadcasted_iota(jnp.int32, values.shape, 0)
    inside = (row >= count) if count > 0 else (row < tokens + count)
    return jnp.where(inside, pltpu.roll(values, count % tokens, 0), 0.0)


def lanes_of(c):
    return pl.ds(pl.multiple_of(c * LANES, LANES), LANES)


def split_rows(out, values, lanes=slice(None)):
    start = 0
    for ref in out:
        rows = ref.shape[0]
        ref[:, lanes] = values[start : start + rows]
        start += rows


def slabs(length, rows, width):
    starts = range(0, length, rows)
    return [pltpu.VMEM((min(rows, length - s), width), jnp.bfloat16) for s in starts]


def whole(array):
    return pl.BlockSpec(array.shape, lambda c, *_: (0,) * len(array.shape))


def conv_kernel(place, gate, up, taps, grad, down, swish_out, slope_out, *refs):
    down_out, act_out = refs[: LANES // DOWN_ROWS], refs[LANES // DOWN_ROWS :]
    share = product(grad[...], down[...], ((1,), (1,))).astype(jnp.bfloat16)
    split_rows(act_out, share, lanes_of(pl.program_id(0)))
    gate_float = gate[...].astype(jnp.float32)
    up_float = up[...].astype(jnp.float32)
    taps_float = taps[...].astype(jnp.float32)
    conv_out = (
        taps_float[0:1] * moved(gate_float, 2)
        + taps_float[1:2] * moved(gate_float, 1)
        + taps_float[2:3] * gate_float
    )
    sig = jax.nn.sigmoid(conv_out)
    swish = conv_out * sig
    swish_out[...] = swish.astype(jnp.bfloat16)
    slope_out[...] = (up_float * sig * (1.0 + conv_out * (1.0 - sig))).astype(jnp.bfloat16)
    activation = (swish * up_float).astype(jnp.bfloat16)
    split_rows(down_out, product(activation, grad[...], ((0,), (0,))).astype(jnp.bfloat16))


def conv_cells(place, gate_saved, up_saved, conv_taps, out_grad, w_down):
    tokens, hidden = gate_saved.shape
    block = w_down.shape[1]
    acts = slabs(tokens, ROWS, hidden)
    columns = pl.BlockSpec((tokens, LANES), lambda c, s: (0, c))
    cells = pltpu.HBM((tokens, hidden), jnp.bfloat16)
    run = LANES // DOWN_ROWS
    down = pltpu.HBM((hidden // run, block), jnp.bfloat16)
    return pl.pallas_call(
        conv_kernel,
        out_shape=[cells, cells] + [down] * run + acts,
        grid_spec=pltpu.PrefetchScalarGridSpec(
            num_scalar_prefetch=1,
            grid=(hidden // LANES,),
            in_specs=[
                columns,
                columns,
                pl.BlockSpec((TAPS, LANES), lambda c, s: (0, c)),
                pl.BlockSpec((tokens, block), lambda c, s: (0, s[0])),
                pl.BlockSpec((LANES, block), lambda c, s: (c, 0)),
            ],
            out_specs=[columns, columns]
            + [pl.BlockSpec((DOWN_ROWS, block), lambda c, s: (c, 0))] * run
            + [whole(a) for a in acts],
        ),
        compiler_params=pltpu.CompilerParams(vmem_limit_bytes=16 << 20),
        name="conv_cells",
    )(place, gate_saved, up_saved, conv_taps, out_grad, w_down)


def taken(refs, counts):
    runs = []
    for count in counts:
        runs.append(refs[:count])
        refs = refs[count:]
    return *runs, refs


def grad_kernel(counts, taps, swish, slope, gate, inputs, w_gate, w_up, *refs):
    acts, downs, _, (terms_out, taps_out), grads_out, down_out, (terms,) = taken(refs, counts)
    c = pl.program_id(0)
    for i, down in enumerate(downs):
        for j in range(len(down_out) // len(downs)):

            @pl.when(c == j)
            def copy(ref=down_out[j * len(downs) + i], down=down):
                ref[...] = down[...]

    act_grad = jnp.concatenate([a[:, lanes_of(c)] for a in acts], 0).astype(jnp.float32)
    up_part = (act_grad * swish[...].astype(jnp.float32)).astype(jnp.bfloat16)
    conv_grad = act_grad * slope[...].astype(jnp.float32)
    taps_float = taps[...].astype(jnp.float32)
    ahead_one, ahead_two = moved(conv_grad, -1), moved(conv_grad, -2)
    gate_part = (
        taps_float[0:1] * ahead_two + taps_float[1:2] * ahead_one + taps_float[2:3] * conv_grad
    ).astype(jnp.bfloat16)
    gate_float = gate[...].astype(jnp.float32)
    sums = [
        jnp.sum(ahead * gate_float, axis=0, keepdims=True)
        for ahead in (ahead_two, ahead_one, conv_grad)
    ]
    taps_out[:, lanes_of(c)] = jnp.concatenate(sums, 0).astype(jnp.bfloat16)
    parts = jnp.concatenate([gate_part, up_part], 1)
    grads = product(inputs[...], parts, ((1,), (0,))).astype(jnp.bfloat16)
    split_rows(grads_out, jnp.concatenate([grads[:, :LANES], grads[:, LANES:]], 0), lanes_of(c))
    weights = jnp.concatenate([w_gate[...], w_up[...]], 1)
    term = product(weights, parts, ((1,), (1,)))

    @pl.when(c == 0)
    def first():
        terms[...] = term

    @pl.when(c > 0)
    def later():
        terms[...] += term

    @pl.when(c == pl.num_programs(0) - 1)
    def last():
        terms_out[...] = terms[...].astype(jnp.bfloat16)


def grad_cells(conv_taps, swish, slope, gate_saved, inputs, w_gate, w_up, acts, downs, extra):
    tokens, hidden = swish.shape
    block = inputs.shape[0]
    columns = pl.BlockSpec((tokens, LANES), lambda c: (0, c))
    weights = pl.BlockSpec((block, LANES), lambda c: (0, c))
    grads = slabs(2 * block, ROWS, hidden)
    kept = slabs(hidden, DOWN_ROWS, block)
    out = [
        pltpu.HBM((block, tokens), jnp.bfloat16),
        pltpu.VMEM((TAPS, hidden), jnp.bfloat16),
    ] + grads + kept
    counts = [len(acts), len(downs), 1, 2, len(grads), len(kept)]
    return pl.pallas_call(
        lambda *refs: grad_kernel(counts, *refs),
        out_shape=out,
        grid=(hidden // LANES,),
        in_specs=[pl.BlockSpec((TAPS, LANES), lambda c: (0, c)), columns, columns, columns]
        + [whole(inputs), weights, weights]
        + [whole(a) for a in acts]
        + [pl.BlockSpec((DOWN_ROWS, block), lambda c: (c, 0))] * len(downs)
        + [pl.BlockSpec(memory_space=pl.ANY)],
        out_specs=[whole(o) for o in out],
        scratch_shapes=[pltpu.VMEM((block, tokens), jnp.float32)],
        compiler_params=pltpu.CompilerParams(vmem_limit_bytes=24 << 20),
        name="grad_cells",
    )(conv_taps, swish, slope, gate_saved, inputs, w_gate, w_up, *acts, *downs, extra)


def widen_kernel(counts, *refs):
    pairs, downs, (taps, _), (gate_out, up_out, down_out, taps_out) = taken(refs, counts)
    block = gate_out.shape[0]
    start = 0
    for ref in pairs:
        rows = ref.shape[0]
        values = ref[...].astype(jnp.float32)
        cut = min(max(block - start, 0), rows)
        if cut > 0:
            gate_out[start : start + cut, :] = values[:cut]
        if cut < rows:
            up_out[start + cut - block : start + rows - block, :] = values[cut:]
        start += rows
    for i, ref in enumerate(downs):
        down_out[i * DOWN_ROWS : (i + 1) * DOWN_ROWS, :] = ref[...].astype(jnp.float32)
    taps_out[...] = taps[...].astype(jnp.float32)


def widened(pairs, downs, taps, extra):
    hidden = taps.shape[1]
    block = downs[0].shape[1]
    grads = jax.ShapeDtypeStruct((block, hidden), jnp.float32)
    counts = [len(pairs), len(downs), 2]
    return pl.pallas_call(
        lambda *refs: widen_kernel(counts, *refs),
        out_shape=[
            grads,
            grads,
            jax.ShapeDtypeStruct((hidden, block), jnp.float32),
            jax.ShapeDtypeStruct((TAPS, hidden), jnp.float32),
        ],
        in_specs=[pl.BlockSpec(memory_space=pltpu.VMEM)] * (sum(counts) - 1)
        + [pl.BlockSpec(memory_space=pl.ANY)],
        compiler_params=pltpu.CompilerParams(vmem_limit_bytes=16 << 20),
        name="widened",
    )(*pairs, *downs, taps, extra)


def local(layer_input, gate_saved, up_saved, out_grad, conv_taps, w_gate, w_up, w_down):
    gate_saved, up_saved, out_grad, w_gate, w_up, w_down = [
        pltpu.with_memory_space_constraint(a, pltpu.HBM)
        for a in (gate_saved, up_saved, out_grad, w_gate, w_up, w_down)
    ]
    tp = lax.axis_size("tp")
    tokens = out_grad.shape[0]
    block = w_gate.shape[0]
    place = lax.axis_index("fs").astype(jnp.int32).reshape(1)
    inputs = jnp.broadcast_to(layer_input.T[None], (tp, block // tp, tokens))
    inputs = lax.all_to_all(inputs, "tp", 0, 0, tiled=True).reshape(block, tokens)
    run = LANES // DOWN_ROWS
    swish, slope, *rest = conv_cells(place, gate_saved, up_saved, conv_taps, out_grad, w_down)
    downs, acts = rest[:run], rest[run:]
    scalar = conv_taps[0, 0]
    *acts, extra = lax.psum([*acts, scalar], "fs")
    acts = [pltpu.with_memory_space_constraint(a, pltpu.VMEM) for a in acts]
    inputs, swish, slope, *downs = [
        pltpu.with_memory_space_constraint(a, pltpu.HBM) for a in (inputs, swish, slope, *downs)
    ]
    terms, taps, *grads = grad_cells(
        conv_taps, swish, slope, gate_saved, inputs, w_gate, w_up, acts, downs, extra.reshape(1, 1)
    )
    terms = lax.all_to_all(terms.reshape(tp, block // tp, tokens), "tp", 0, 0, tiled=True)
    input_grad = jnp.sum(terms.astype(jnp.float32), axis=0).astype(jnp.bfloat16).T
    *grads, taps, extra = lax.psum([*grads, taps, scalar], "rep")
    *grads, taps = [pltpu.with_memory_space_constraint(a, pltpu.VMEM) for a in (*grads, taps)]
    count = -(-2 * block // ROWS)
    gate_grad, up_grad, down_grad, taps_grad = widened(
        grads[:count], grads[count:], taps, extra.reshape(1, 1)
    )
    return (input_grad, gate_grad, up_grad, down_grad, taps_grad)


def solution(mesh):
    placed = (
        P("rep", ("fs", "tp")),
        P("rep", "tp"),
        P("rep", "tp"),
        P("rep", None),
        P(None, "tp"),
        P("fs", "tp"),
        P("fs", "tp"),
        P("tp", "fs"),
    )
    return jax.shard_map(
        local,
        mesh=mesh,
        in_specs=placed,
        out_specs=(
            P("rep", ("fs", "tp")),
            P("fs", "tp"),
            P("fs", "tp"),
            P("tp", "fs"),
            P(None, "tp"),
        ),
        check_vma=False,
    )
```

```python
import jax
import jax.numpy as jnp
from jax import lax
from jax.experimental import pallas as pl
from jax.experimental.pallas import tpu as pltpu
from jax.sharding import PartitionSpec as P

LANES = 128
ROWS = 48
DOWN_ROWS = 64
TAPS = 3


def product(left, right, dims):
    return lax.dot_general(left, right, (dims, ((), ())), preferred_element_type=jnp.float32)


def moved(values, count):
    tokens = values.shape[0]
    turned = pltpu.roll(values, count % tokens, 0)
    row = lax.broadcasted_iota(jnp.int32, (8, values.shape[1]), 0)
    if count > 0:
        return jnp.concatenate([jnp.where(row >= count, turned[:8], 0.0), turned[8:]], 0)
    return jnp.concatenate([turned[:-8], jnp.where(row < 8 + count, turned[-8:], 0.0)], 0)


def lanes_of(c):
    return pl.ds(pl.multiple_of(c * LANES, LANES), LANES)


def split_rows(out, values, lanes=slice(None)):
    start = 0
    for ref in out:
        rows = ref.shape[0]
        ref[:, lanes] = values[start : start + rows]
        start += rows


def slabs(length, rows, width):
    starts = range(0, length, rows)
    return [pltpu.VMEM((min(rows, length - s), width), jnp.bfloat16) for s in starts]


def whole(array):
    return pl.BlockSpec(array.shape, lambda c, *_: (0,) * len(array.shape))


def conv_kernel(place, gate, up, taps, grad, down, inputs, *refs):
    swish_out, slope_out, copies_out, one_out = refs[:4]
    down_out, act_out = refs[4 : 4 + LANES // DOWN_ROWS], refs[4 + LANES // DOWN_ROWS :]

    @pl.when(pl.program_id(0) == 0)
    def first():
        one_out[...] = taps[0:1, 0:1]
        for i in range(copies_out.shape[0]):
            copies_out[i] = inputs[...]

    share = product(grad[...], down[...], ((1,), (1,))).astype(jnp.bfloat16)
    split_rows(act_out, share, lanes_of(pl.program_id(0)))
    gate_float = gate[...].astype(jnp.float32)
    up_float = up[...].astype(jnp.float32)
    taps_float = taps[...].astype(jnp.float32)
    conv_out = (
        taps_float[0:1] * moved(gate_float, 2)
        + taps_float[1:2] * moved(gate_float, 1)
        + taps_float[2:3] * gate_float
    )
    sig = 0.5 * jnp.tanh(0.5 * conv_out) + 0.5
    swish = conv_out * sig
    swish_out[...] = swish.astype(jnp.bfloat16)
    slope_out[...] = (up_float * (sig + swish * (1.0 - sig))).astype(jnp.bfloat16)
    activation = (swish * up_float).astype(jnp.bfloat16)
    split_rows(down_out, product(activation, grad[...], ((0,), (0,))).astype(jnp.bfloat16))


def conv_cells(place, gate_saved, up_saved, conv_taps, out_grad, w_down, inputs, copies):
    tokens, hidden = gate_saved.shape
    block = w_down.shape[1]
    acts = slabs(tokens, ROWS, hidden)
    columns = pl.BlockSpec((tokens, LANES), lambda c, s: (0, c))
    cells = pltpu.HBM((tokens, hidden), jnp.bfloat16)
    copies = pltpu.HBM((copies, *inputs.shape), inputs.dtype)
    one = jax.ShapeDtypeStruct((1, 1), jnp.bfloat16)
    run = LANES // DOWN_ROWS
    down = pltpu.HBM((hidden // run, block), jnp.bfloat16)
    return pl.pallas_call(
        conv_kernel,
        out_shape=[cells, cells, copies, one] + [down] * run + acts,
        grid_spec=pltpu.PrefetchScalarGridSpec(
            num_scalar_prefetch=1,
            grid=(hidden // LANES,),
            in_specs=[
                columns,
                columns,
                pl.BlockSpec((TAPS, LANES), lambda c, s: (0, c)),
                pl.BlockSpec((tokens, block), lambda c, s: (0, s[0])),
                pl.BlockSpec((LANES, block), lambda c, s: (c, 0)),
                whole(inputs),
            ],
            out_specs=[columns, columns, whole(copies), whole(one)]
            + [pl.BlockSpec((DOWN_ROWS, block), lambda c, s: (c, 0))] * run
            + [whole(a) for a in acts],
        ),
        compiler_params=pltpu.CompilerParams(vmem_limit_bytes=16 << 20),
        name="conv_cells",
    )(place, gate_saved, up_saved, conv_taps, out_grad, w_down, inputs)


def taken(refs, counts):
    runs = []
    for count in counts:
        runs.append(refs[:count])
        refs = refs[count:]
    return *runs, refs


def grad_kernel(counts, taps, swish, slope, gate, inputs, w_gate, w_up, *refs):
    acts, downs, _, (terms_out, taps_out), grads_out, down_out, (terms,) = taken(refs, counts)
    c = pl.program_id(0)
    for i, down in enumerate(downs):
        for j in range(len(down_out) // len(downs)):

            @pl.when(c == j)
            def copy(ref=down_out[j * len(downs) + i], down=down):
                ref[...] = down[...]

    act_grad = jnp.concatenate([a[:, lanes_of(c)] for a in acts], 0).astype(jnp.float32)
    up_part = (act_grad * swish[...].astype(jnp.float32)).astype(jnp.bfloat16)
    conv_grad = act_grad * slope[...].astype(jnp.float32)
    taps_float = taps[...].astype(jnp.float32)
    ahead_one, ahead_two = moved(conv_grad, -1), moved(conv_grad, -2)
    gate_part = (
        taps_float[0:1] * ahead_two + taps_float[1:2] * ahead_one + taps_float[2:3] * conv_grad
    ).astype(jnp.bfloat16)
    gate_float = gate[...].astype(jnp.float32)
    sums = [
        jnp.sum(ahead * gate_float, axis=0, keepdims=True)
        for ahead in (ahead_two, ahead_one, conv_grad)
    ]
    taps_out[:, lanes_of(c)] = jnp.concatenate(sums, 0).astype(jnp.bfloat16)
    parts = jnp.concatenate([gate_part, up_part], 1)
    grads = product(inputs[...], parts, ((1,), (0,))).astype(jnp.bfloat16)
    split_rows(grads_out, jnp.concatenate([grads[:, :LANES], grads[:, LANES:]], 0), lanes_of(c))
    weights = jnp.concatenate([w_gate[...], w_up[...]], 1)
    term = product(weights, parts, ((1,), (1,)))

    @pl.when(c == 0)
    def first():
        terms[...] = term

    @pl.when(c > 0)
    def later():
        terms[...] += term

    @pl.when(c == pl.num_programs(0) - 1)
    def last():
        terms_out[...] = terms[...].astype(jnp.bfloat16)


def grad_cells(conv_taps, swish, slope, gate_saved, inputs, w_gate, w_up, acts, downs, extra):
    tokens, hidden = swish.shape
    block = inputs.shape[0]
    columns = pl.BlockSpec((tokens, LANES), lambda c: (0, c))
    weights = pl.BlockSpec((block, LANES), lambda c: (0, c))
    grads = slabs(2 * block, ROWS, hidden)
    kept = slabs(hidden, DOWN_ROWS, block)
    out = [
        pltpu.HBM((block, tokens), jnp.bfloat16),
        pltpu.VMEM((TAPS, hidden), jnp.bfloat16),
    ] + grads + kept
    counts = [len(acts), len(downs), 1, 2, len(grads), len(kept)]
    return pl.pallas_call(
        lambda *refs: grad_kernel(counts, *refs),
        out_shape=out,
        grid=(hidden // LANES,),
        in_specs=[pl.BlockSpec((TAPS, LANES), lambda c: (0, c)), columns, columns, columns]
        + [whole(inputs), weights, weights]
        + [whole(a) for a in acts]
        + [pl.BlockSpec((DOWN_ROWS, block), lambda c: (c, 0))] * len(downs)
        + [pl.BlockSpec(memory_space=pl.ANY)],
        out_specs=[whole(o) for o in out],
        scratch_shapes=[pltpu.VMEM((block, tokens), jnp.float32)],
        compiler_params=pltpu.CompilerParams(vmem_limit_bytes=24 << 20),
        name="grad_cells",
    )(conv_taps, swish, slope, gate_saved, inputs, w_gate, w_up, *acts, *downs, extra)


def widen_kernel(counts, *refs):
    pairs, downs, (taps, _), (gate_out, up_out, down_out, taps_out) = taken(refs, counts)
    block = gate_out.shape[0]
    start = 0
    for ref in pairs:
        rows = ref.shape[0]
        values = ref[...].astype(jnp.float32)
        cut = min(max(block - start, 0), rows)
        if cut > 0:
            gate_out[start : start + cut, :] = values[:cut]
        if cut < rows:
            up_out[start + cut - block : start + rows - block, :] = values[cut:]
        start += rows
    for i, ref in enumerate(downs):
        down_out[i * DOWN_ROWS : (i + 1) * DOWN_ROWS, :] = ref[...].astype(jnp.float32)
    taps_out[...] = taps[...].astype(jnp.float32)


def widened(pairs, downs, taps, extra):
    hidden = taps.shape[1]
    block = downs[0].shape[1]
    grads = jax.ShapeDtypeStruct((block, hidden), jnp.float32)
    counts = [len(pairs), len(downs), 2]
    return pl.pallas_call(
        lambda *refs: widen_kernel(counts, *refs),
        out_shape=[
            grads,
            grads,
            jax.ShapeDtypeStruct((hidden, block), jnp.float32),
            jax.ShapeDtypeStruct((TAPS, hidden), jnp.float32),
        ],
        in_specs=[pl.BlockSpec(memory_space=pltpu.VMEM)] * (sum(counts) - 1)
        + [pl.BlockSpec(memory_space=pl.ANY)],
        compiler_params=pltpu.CompilerParams(vmem_limit_bytes=16 << 20),
        name="widened",
    )(*pairs, *downs, taps, extra)


def local(layer_input, gate_saved, up_saved, out_grad, conv_taps, w_gate, w_up, w_down):
    layer_input, gate_saved, up_saved, out_grad, conv_taps, w_gate, w_up, w_down = [
        pltpu.with_memory_space_constraint(a, pltpu.HBM)
        for a in (layer_input.T, gate_saved, up_saved, out_grad, conv_taps, w_gate, w_up, w_down)
    ]
    tp = lax.axis_size("tp")
    tokens = out_grad.shape[0]
    block = w_gate.shape[0]
    place = lax.axis_index("fs").astype(jnp.int32).reshape(1)
    run = LANES // DOWN_ROWS
    swish, slope, copies, one, *rest = conv_cells(
        place, gate_saved, up_saved, conv_taps, out_grad, w_down, layer_input, tp
    )
    downs, acts = rest[:run], rest[run:]
    inputs = lax.all_to_all(copies, "tp", 0, 0, tiled=True).reshape(block, tokens)
    *acts, extra = lax.psum([*acts, one], "fs")
    acts = [pltpu.with_memory_space_constraint(a, pltpu.VMEM) for a in acts]
    inputs = pltpu.with_memory_space_constraint(inputs, pltpu.VMEM)
    swish, slope, *downs = [
        pltpu.with_memory_space_constraint(a, pltpu.HBM) for a in (swish, slope, *downs)
    ]
    terms, taps, *grads = grad_cells(
        conv_taps, swish, slope, gate_saved, inputs, w_gate, w_up, acts, downs, extra
    )
    terms = lax.all_to_all(terms.reshape(tp, block // tp, tokens), "tp", 0, 0, tiled=True)
    input_grad = jnp.sum(terms.astype(jnp.float32), axis=0).astype(jnp.bfloat16).T
    *grads, taps, extra = lax.psum([*grads, taps, one], "rep")
    *grads, taps = [pltpu.with_memory_space_constraint(a, pltpu.VMEM) for a in (*grads, taps)]
    count = -(-2 * block // ROWS)
    gate_grad, up_grad, down_grad, taps_grad = widened(
        grads[:count], grads[count:], taps, extra
    )
    return (input_grad, gate_grad, up_grad, down_grad, taps_grad)


def solution(mesh):
    placed = (
        P("rep", ("fs", "tp")),
        P("rep", "tp"),
        P("rep", "tp"),
        P("rep", None),
        P(None, "tp"),
        P("fs", "tp"),
        P("fs", "tp"),
        P("tp", "fs"),
    )
    return jax.shard_map(
        local,
        mesh=mesh,
        in_specs=placed,
        out_specs=(
            P("rep", ("fs", "tp")),
            P("fs", "tp"),
            P("fs", "tp"),
            P("tp", "fs"),
            P(None, "tp"),
        ),
        check_vma=False,
    )
```

```python
import jax
import jax.numpy as jnp
from jax import lax
from jax.experimental import pallas as pl
from jax.experimental.pallas import tpu as pltpu
from jax.sharding import PartitionSpec as P

LANES = 128
ROWS = 48
DOWN_ROWS = 120
TAPS = 3


def product(left, right, dims):
    return lax.dot_general(left, right, (dims, ((), ())), preferred_element_type=jnp.float32)


def moved(values, count):
    tokens = values.shape[0]
    turned = pltpu.roll(values, count % tokens, 0)
    row = lax.broadcasted_iota(jnp.int32, (8, values.shape[1]), 0)
    if count > 0:
        return jnp.concatenate([jnp.where(row >= count, turned[:8], 0.0), turned[8:]], 0)
    return jnp.concatenate([turned[:-8], jnp.where(row < 8 + count, turned[-8:], 0.0)], 0)


def lanes_of(c):
    return pl.ds(pl.multiple_of(c * LANES, LANES), LANES)


def split_rows(out, values, lanes=slice(None)):
    start = 0
    for ref in out:
        rows = ref.shape[0]
        ref[:, lanes] = values[start : start + rows, :]
        start += rows


def slabs(length, rows, width):
    starts = range(0, length, rows)
    return [pltpu.VMEM((min(rows, length - s), width), jnp.bfloat16) for s in starts]


def whole(array):
    return pl.BlockSpec(array.shape, lambda c, *_: (0,) * len(array.shape))


def conv_kernel(place, gate, up, taps, grad, down, inputs, *refs):
    swish_out, slope_out, copies_out, one_out, down_out, *act_out = refs

    @pl.when(pl.program_id(0) == 0)
    def first():
        one_out[...] = taps[0:1, 0:1]
        for i in range(copies_out.shape[0]):
            copies_out[i] = inputs[...]

    share = product(grad[...], down[...], ((1,), (1,))).astype(jnp.bfloat16)
    split_rows(act_out, share, lanes_of(pl.program_id(0)))
    gate_float = gate[...].astype(jnp.float32)
    up_float = up[...].astype(jnp.float32)
    taps_float = taps[...].astype(jnp.float32)
    conv_out = (
        taps_float[0:1] * moved(gate_float, 2)
        + taps_float[1:2] * moved(gate_float, 1)
        + taps_float[2:3] * gate_float
    )
    sig = 0.5 * jnp.tanh(0.5 * conv_out) + 0.5
    swish = conv_out * sig
    swish_out[...] = swish.astype(jnp.bfloat16)
    slope_out[...] = (up_float * (sig + swish * (1.0 - sig))).astype(jnp.bfloat16)
    activation = (swish * up_float).astype(jnp.bfloat16)
    down_out[...] = product(activation, grad[...], ((0,), (0,))).astype(jnp.bfloat16)


def conv_cells(place, gate_saved, up_saved, conv_taps, out_grad, w_down, inputs, copies):
    tokens, hidden = gate_saved.shape
    block = w_down.shape[1]
    acts = slabs(tokens, ROWS, hidden)
    columns = pl.BlockSpec((tokens, LANES), lambda c, s: (0, c))
    cells = pltpu.HBM((tokens, hidden), jnp.bfloat16)
    copies = pltpu.HBM((copies, *inputs.shape), inputs.dtype)
    one = jax.ShapeDtypeStruct((1, 1), jnp.bfloat16)
    down = pltpu.HBM((hidden, block), jnp.bfloat16)
    return pl.pallas_call(
        conv_kernel,
        out_shape=[cells, cells, copies, one, down] + acts,
        grid_spec=pltpu.PrefetchScalarGridSpec(
            num_scalar_prefetch=1,
            grid=(hidden // LANES,),
            in_specs=[
                columns,
                columns,
                pl.BlockSpec((TAPS, LANES), lambda c, s: (0, c)),
                pl.BlockSpec((tokens, block), lambda c, s: (0, s[0])),
                pl.BlockSpec((LANES, block), lambda c, s: (c, 0)),
                whole(inputs),
            ],
            out_specs=[columns, columns, whole(copies), whole(one)]
            + [pl.BlockSpec((LANES, block), lambda c, s: (c, 0))]
            + [whole(a) for a in acts],
        ),
        compiler_params=pltpu.CompilerParams(vmem_limit_bytes=16 << 20),
        name="conv_cells",
    )(place, gate_saved, up_saved, conv_taps, out_grad, w_down, inputs)


def taken(refs, counts):
    runs = []
    for count in counts:
        runs.append(refs[:count])
        refs = refs[count:]
    return *runs, refs


def grad_kernel(counts, taps, swish, slope, gate, inputs, w_gate, w_up, *refs):
    acts, (down, _, terms_out), grads_out, down_out, (terms,) = taken(refs, counts)
    c = pl.program_id(0)

    @pl.when(c == 0)
    def copy():
        split_rows(down_out, down)

    act_grad = jnp.concatenate([a[:, lanes_of(c)] for a in acts], 0).astype(jnp.float32)
    up_part = (act_grad * swish[...].astype(jnp.float32)).astype(jnp.bfloat16)
    conv_grad = act_grad * slope[...].astype(jnp.float32)
    taps_float = taps[...].astype(jnp.float32)
    ahead_one, ahead_two = moved(conv_grad, -1), moved(conv_grad, -2)
    gate_part = (
        taps_float[0:1] * ahead_two + taps_float[1:2] * ahead_one + taps_float[2:3] * conv_grad
    ).astype(jnp.bfloat16)
    gate_float = gate[...].astype(jnp.float32)
    sums = [
        jnp.sum(ahead * gate_float, axis=0, keepdims=True)
        for ahead in (ahead_two, ahead_one, conv_grad)
    ]
    sums = jnp.concatenate(sums + [jnp.zeros((8 - TAPS, LANES), jnp.float32)], 0)
    parts = jnp.concatenate([gate_part, up_part], 1)
    grads = product(inputs[...], parts, ((1,), (0,))).astype(jnp.bfloat16)
    columns = [grads[:, :LANES], grads[:, LANES:], sums.astype(jnp.bfloat16)]
    split_rows(grads_out, jnp.concatenate(columns, 0), lanes_of(c))
    weights = jnp.concatenate([w_gate[...], w_up[...]], 1)
    term = product(weights, parts, ((1,), (1,)))

    @pl.when(c == 0)
    def first():
        terms[...] = term

    @pl.when(c > 0)
    def later():
        terms[...] += term

    @pl.when(c == pl.num_programs(0) - 1)
    def last():
        terms_out[...] = terms[...].astype(jnp.bfloat16)


def grad_cells(conv_taps, swish, slope, gate_saved, inputs, w_gate, w_up, acts, down, extra):
    tokens, hidden = swish.shape
    block = inputs.shape[0]
    columns = pl.BlockSpec((tokens, LANES), lambda c: (0, c))
    weights = pl.BlockSpec((block, LANES), lambda c: (0, c))
    grads = slabs(2 * block + 8, ROWS, hidden)
    kept = slabs(hidden, DOWN_ROWS, block)
    out = [pltpu.HBM((block, tokens), jnp.bfloat16)] + grads + kept
    counts = [len(acts), 3, len(grads), len(kept)]
    return pl.pallas_call(
        lambda *refs: grad_kernel(counts, *refs),
        out_shape=out,
        grid=(hidden // LANES,),
        in_specs=[pl.BlockSpec((TAPS, LANES), lambda c: (0, c)), columns, columns, columns]
        + [whole(inputs), weights, weights]
        + [whole(a) for a in acts]
        + [whole(down), pl.BlockSpec(memory_space=pl.ANY)],
        out_specs=[whole(o) for o in out],
        scratch_shapes=[pltpu.VMEM((block, tokens), jnp.float32)],
        compiler_params=pltpu.CompilerParams(vmem_limit_bytes=24 << 20),
        name="grad_cells",
    )(conv_taps, swish, slope, gate_saved, inputs, w_gate, w_up, *acts, down, extra)


def widen_kernel(counts, *refs):
    pairs, downs, (terms, _, input_out, gate_out, up_out, down_out, taps_out), _ = taken(refs, counts)
    block = gate_out.shape[0]
    bounds = ((gate_out, 0, block), (up_out, block, 2 * block), (taps_out, 2 * block, 2 * block + TAPS))
    start = 0
    for ref in pairs:
        values = ref[...].astype(jnp.float32)
        for out, low, high in bounds:
            first, last = max(low, start), min(high, start + ref.shape[0])
            if first < last:
                out[first - low : last - low, :] = values[first - start : last - start]
        start += ref.shape[0]
    start = 0
    for ref in downs:
        down_out[start : start + ref.shape[0], :] = ref[...].astype(jnp.float32)
        start += ref.shape[0]
    total = terms[0].astype(jnp.float32)
    for i in range(1, terms.shape[0]):
        total = total + terms[i].astype(jnp.float32)
    input_out[...] = total.astype(jnp.bfloat16)


def widened(pairs, downs, terms, extra):
    hidden = pairs[0].shape[1]
    block = downs[0].shape[1]
    grads = jax.ShapeDtypeStruct((block, hidden), jnp.float32)
    counts = [len(pairs), len(downs), 7]
    return pl.pallas_call(
        lambda *refs: widen_kernel(counts, *refs),
        out_shape=[
            jax.ShapeDtypeStruct(terms.shape[1:], jnp.bfloat16),
            grads,
            grads,
            jax.ShapeDtypeStruct((hidden, block), jnp.float32),
            jax.ShapeDtypeStruct((TAPS, hidden), jnp.float32),
        ],
        in_specs=[pl.BlockSpec(memory_space=pltpu.VMEM)] * (len(pairs) + len(downs) + 1)
        + [pl.BlockSpec(memory_space=pl.ANY)],
        compiler_params=pltpu.CompilerParams(vmem_limit_bytes=16 << 20),
        name="widened",
    )(*pairs, *downs, terms, extra)


def local(layer_input, gate_saved, up_saved, out_grad, conv_taps, w_gate, w_up, w_down):
    layer_input, gate_saved, up_saved, out_grad, conv_taps, w_gate, w_up, w_down = [
        pltpu.with_memory_space_constraint(a, pltpu.HBM)
        for a in (layer_input.T, gate_saved, up_saved, out_grad, conv_taps, w_gate, w_up, w_down)
    ]
    tp = lax.axis_size("tp")
    tokens = out_grad.shape[0]
    block = w_gate.shape[0]
    place = lax.axis_index("fs").astype(jnp.int32).reshape(1)
    swish, slope, copies, one, down, *acts = conv_cells(
        place, gate_saved, up_saved, conv_taps, out_grad, w_down, layer_input, tp
    )
    inputs = lax.all_to_all(copies, "tp", 0, 0, tiled=True).reshape(block, tokens)
    *acts, extra = lax.psum([*acts, one], "fs")
    acts = [pltpu.with_memory_space_constraint(a, pltpu.VMEM) for a in acts]
    inputs = pltpu.with_memory_space_constraint(inputs, pltpu.VMEM)
    swish, slope, down = [
        pltpu.with_memory_space_constraint(a, pltpu.HBM) for a in (swish, slope, down)
    ]
    terms, *grads = grad_cells(
        conv_taps, swish, slope, gate_saved, inputs, w_gate, w_up, acts, down, extra
    )
    terms = lax.all_to_all(terms.reshape(tp, block // tp, tokens), "tp", 0, 0, tiled=True)
    *grads, extra = lax.psum([*grads, one], "rep")
    grads = [pltpu.with_memory_space_constraint(a, pltpu.VMEM) for a in grads]
    count = len(slabs(2 * block + 8, ROWS, 1))
    input_grad, gate_grad, up_grad, down_grad, taps_grad = widened(
        grads[:count], grads[count:], terms, extra
    )
    return (input_grad.T, gate_grad, up_grad, down_grad, taps_grad)


def solution(mesh):
    placed = (
        P("rep", ("fs", "tp")),
        P("rep", "tp"),
        P("rep", "tp"),
        P("rep", None),
        P(None, "tp"),
        P("fs", "tp"),
        P("fs", "tp"),
        P("tp", "fs"),
    )
    return jax.shard_map(
        local,
        mesh=mesh,
        in_specs=placed,
        out_specs=(
            P("rep", ("fs", "tp")),
            P("fs", "tp"),
            P("fs", "tp"),
            P("tp", "fs"),
            P(None, "tp"),
        ),
        check_vma=False,
    )
```

```python
import jax
import jax.numpy as jnp
from jax import lax
from jax.experimental import pallas as pl
from jax.experimental.pallas import tpu as pltpu
from jax.sharding import PartitionSpec as P

LANES = 128
ROWS = 48
DOWN_ROWS = 120
TAPS = 3


def product(left, right, dims):
    return lax.dot_general(left, right, (dims, ((), ())), preferred_element_type=jnp.float32)


def moved(values, count):
    tokens = values.shape[0]
    turned = pltpu.roll(values, count % tokens, 0)
    row = lax.broadcasted_iota(jnp.int32, (8, values.shape[1]), 0)
    if count > 0:
        return jnp.concatenate([jnp.where(row >= count, turned[:8], 0.0), turned[8:]], 0)
    return jnp.concatenate([turned[:-8], jnp.where(row < 8 + count, turned[-8:], 0.0)], 0)


def lanes_of(c):
    return slice(c * LANES, (c + 1) * LANES)


def split_rows(out, values, lanes=slice(None)):
    start = 0
    for ref in out:
        rows = ref.shape[0]
        ref[:, lanes] = values[start : start + rows, :]
        start += rows


def slabs(length, rows, width):
    starts = range(0, length, rows)
    return [pltpu.VMEM((min(rows, length - s), width), jnp.bfloat16) for s in starts]


def whole(array):
    return pl.BlockSpec(array.shape, lambda c, *_: (0,) * len(array.shape))


def conv_kernel(place, gate, up, taps, grad, down, inputs, *refs):
    swish_out, slope_out, copies_out, one_out, down_out, *act_out = refs
    one_out[...] = taps[0:1, 0:1]
    for i in range(copies_out.shape[0]):
        copies_out[i] = inputs[...]
    for c in range(gate.shape[1] // LANES):
        lanes = lanes_of(c)
        share = product(grad[...], down[lanes, :], ((1,), (1,))).astype(jnp.bfloat16)
        split_rows(act_out, share, lanes)
        gate_float = gate[:, lanes].astype(jnp.float32)
        up_float = up[:, lanes].astype(jnp.float32)
        taps_float = taps[:, lanes].astype(jnp.float32)
        conv_out = (
            taps_float[0:1] * moved(gate_float, 2)
            + taps_float[1:2] * moved(gate_float, 1)
            + taps_float[2:3] * gate_float
        )
        sig = 0.5 * jnp.tanh(0.5 * conv_out) + 0.5
        swish = conv_out * sig
        swish_out[:, lanes] = swish.astype(jnp.bfloat16)
        slope_out[:, lanes] = (up_float * (sig + swish * (1.0 - sig))).astype(jnp.bfloat16)
        activation = (swish * up_float).astype(jnp.bfloat16)
        down_out[lanes, :] = product(activation, grad[...], ((0,), (0,))).astype(jnp.bfloat16)


def conv_cells(place, gate_saved, up_saved, conv_taps, out_grad, w_down, inputs, copies):
    tokens, hidden = gate_saved.shape
    block = w_down.shape[1]
    acts = slabs(tokens, ROWS, hidden)
    cells = pltpu.HBM((tokens, hidden), jnp.bfloat16)
    copies = pltpu.HBM((copies, *inputs.shape), inputs.dtype)
    one = jax.ShapeDtypeStruct((1, 1), jnp.bfloat16)
    down = pltpu.HBM((hidden, block), jnp.bfloat16)
    return pl.pallas_call(
        conv_kernel,
        out_shape=[cells, cells, copies, one, down] + acts,
        grid_spec=pltpu.PrefetchScalarGridSpec(
            num_scalar_prefetch=1,
            grid=(1,),
            in_specs=[
                whole(gate_saved),
                whole(up_saved),
                whole(conv_taps),
                pl.BlockSpec((tokens, block), lambda c, s: (0, s[0])),
                whole(w_down),
                whole(inputs),
            ],
            out_specs=[whole(a) for a in (cells, cells, copies, one, down)]
            + [whole(a) for a in acts],
        ),
        compiler_params=pltpu.CompilerParams(vmem_limit_bytes=32 << 20),
        name="conv_cells",
    )(place, gate_saved, up_saved, conv_taps, out_grad, w_down, inputs)


def taken(refs, counts):
    runs = []
    for count in counts:
        runs.append(refs[:count])
        refs = refs[count:]
    return *runs, refs


def grad_kernel(counts, taps, swish, slope, gate, inputs, w_gate, w_up, *refs):
    acts, (down, _, terms_out), grads_out, down_out, (terms,) = taken(refs, counts)
    split_rows(down_out, down)
    count = swish.shape[1] // LANES
    for c in range(count):
        lanes = lanes_of(c)
        act_grad = jnp.concatenate([a[:, lanes] for a in acts], 0).astype(jnp.float32)
        up_part = (act_grad * swish[:, lanes].astype(jnp.float32)).astype(jnp.bfloat16)
        conv_grad = act_grad * slope[:, lanes].astype(jnp.float32)
        taps_float = taps[:, lanes].astype(jnp.float32)
        ahead_one, ahead_two = moved(conv_grad, -1), moved(conv_grad, -2)
        gate_part = (
            taps_float[0:1] * ahead_two + taps_float[1:2] * ahead_one + taps_float[2:3] * conv_grad
        ).astype(jnp.bfloat16)
        gate_float = gate[:, lanes].astype(jnp.float32)
        sums = [
            jnp.sum(ahead * gate_float, axis=0, keepdims=True)
            for ahead in (ahead_two, ahead_one, conv_grad)
        ]
        sums = jnp.concatenate(sums + [jnp.zeros((8 - TAPS, LANES), jnp.float32)], 0)
        parts = jnp.concatenate([gate_part, up_part], 1)
        grads = product(inputs[...], parts, ((1,), (0,))).astype(jnp.bfloat16)
        columns = [grads[:, :LANES], grads[:, LANES:], sums.astype(jnp.bfloat16)]
        split_rows(grads_out, jnp.concatenate(columns, 0), lanes)
        weights = jnp.concatenate([w_gate[:, lanes], w_up[:, lanes]], 1)
        term = product(weights, parts, ((1,), (1,)))
        if c == 0:
            terms[...] = term
        elif c < count - 1:
            terms[...] += term
        else:
            terms_out[...] = (terms[...] + term).astype(jnp.bfloat16)


def grad_cells(conv_taps, swish, slope, gate_saved, inputs, w_gate, w_up, acts, down, extra):
    tokens, hidden = swish.shape
    block = inputs.shape[0]
    grads = slabs(2 * block + 8, ROWS, hidden)
    kept = slabs(hidden, DOWN_ROWS, block)
    out = [pltpu.HBM((block, tokens), jnp.bfloat16)] + grads + kept
    counts = [len(acts), 3, len(grads), len(kept)]
    return pl.pallas_call(
        lambda *refs: grad_kernel(counts, *refs),
        out_shape=out,
        grid=(1,),
        in_specs=[whole(a) for a in (conv_taps, swish, slope, gate_saved, inputs, w_gate, w_up)]
        + [whole(a) for a in acts]
        + [whole(down), pl.BlockSpec(memory_space=pl.ANY)],
        out_specs=[whole(o) for o in out],
        scratch_shapes=[pltpu.VMEM((block, tokens), jnp.float32)],
        compiler_params=pltpu.CompilerParams(vmem_limit_bytes=32 << 20),
        name="grad_cells",
    )(conv_taps, swish, slope, gate_saved, inputs, w_gate, w_up, *acts, down, extra)


def widen_kernel(counts, *refs):
    pairs, downs, (terms, _, input_out, gate_out, up_out, down_out, taps_out), _ = taken(refs, counts)
    block = gate_out.shape[0]
    bounds = ((gate_out, 0, block), (up_out, block, 2 * block), (taps_out, 2 * block, 2 * block + TAPS))
    start = 0
    for ref in pairs:
        values = ref[...].astype(jnp.float32)
        for out, low, high in bounds:
            first, last = max(low, start), min(high, start + ref.shape[0])
            if first < last:
                out[first - low : last - low, :] = values[first - start : last - start]
        start += ref.shape[0]
    start = 0
    for ref in downs:
        down_out[start : start + ref.shape[0], :] = ref[...].astype(jnp.float32)
        start += ref.shape[0]
    total = terms[0].astype(jnp.float32)
    for i in range(1, terms.shape[0]):
        total = total + terms[i].astype(jnp.float32)
    input_out[...] = total.astype(jnp.bfloat16)


def widened(pairs, downs, terms, extra):
    hidden = pairs[0].shape[1]
    block = downs[0].shape[1]
    grads = jax.ShapeDtypeStruct((block, hidden), jnp.float32)
    counts = [len(pairs), len(downs), 7]
    return pl.pallas_call(
        lambda *refs: widen_kernel(counts, *refs),
        out_shape=[
            jax.ShapeDtypeStruct(terms.shape[1:], jnp.bfloat16),
            grads,
            grads,
            jax.ShapeDtypeStruct((hidden, block), jnp.float32),
            jax.ShapeDtypeStruct((TAPS, hidden), jnp.float32),
        ],
        in_specs=[pl.BlockSpec(memory_space=pltpu.VMEM)] * (len(pairs) + len(downs) + 1)
        + [pl.BlockSpec(memory_space=pl.ANY)],
        compiler_params=pltpu.CompilerParams(vmem_limit_bytes=16 << 20),
        name="widened",
    )(*pairs, *downs, terms, extra)


def local(layer_input, gate_saved, up_saved, out_grad, conv_taps, w_gate, w_up, w_down):
    layer_input, gate_saved, up_saved, out_grad, conv_taps, w_gate, w_up, w_down = [
        pltpu.with_memory_space_constraint(a, pltpu.HBM)
        for a in (layer_input.T, gate_saved, up_saved, out_grad, conv_taps, w_gate, w_up, w_down)
    ]
    tp = lax.axis_size("tp")
    tokens = out_grad.shape[0]
    block = w_gate.shape[0]
    place = lax.axis_index("fs").astype(jnp.int32).reshape(1)
    swish, slope, copies, one, down, *acts = conv_cells(
        place, gate_saved, up_saved, conv_taps, out_grad, w_down, layer_input, tp
    )
    inputs = lax.all_to_all(copies, "tp", 0, 0, tiled=True).reshape(block, tokens)
    *acts, extra = lax.psum([*acts, one], "fs")
    acts = [pltpu.with_memory_space_constraint(a, pltpu.VMEM) for a in acts]
    inputs = pltpu.with_memory_space_constraint(inputs, pltpu.VMEM)
    swish, slope, down = [
        pltpu.with_memory_space_constraint(a, pltpu.HBM) for a in (swish, slope, down)
    ]
    terms, *grads = grad_cells(
        conv_taps, swish, slope, gate_saved, inputs, w_gate, w_up, acts, down, extra
    )
    terms = lax.all_to_all(terms.reshape(tp, block // tp, tokens), "tp", 0, 0, tiled=True)
    *grads, extra = lax.psum([*grads, one], "rep")
    grads = [pltpu.with_memory_space_constraint(a, pltpu.VMEM) for a in grads]
    count = len(slabs(2 * block + 8, ROWS, 1))
    input_grad, gate_grad, up_grad, down_grad, taps_grad = widened(
        grads[:count], grads[count:], terms, extra
    )
    return (input_grad.T, gate_grad, up_grad, down_grad, taps_grad)


def solution(mesh):
    placed = (
        P("rep", ("fs", "tp")),
        P("rep", "tp"),
        P("rep", "tp"),
        P("rep", None),
        P(None, "tp"),
        P("fs", "tp"),
        P("fs", "tp"),
        P("tp", "fs"),
    )
    return jax.shard_map(
        local,
        mesh=mesh,
        in_specs=placed,
        out_specs=(
            P("rep", ("fs", "tp")),
            P("fs", "tp"),
            P("fs", "tp"),
            P("tp", "fs"),
            P(None, "tp"),
        ),
        check_vma=False,
    )
```

```python
import jax
import jax.numpy as jnp
from jax import lax
from jax.experimental import pallas as pl
from jax.experimental.pallas import tpu as pltpu
from jax.sharding import PartitionSpec as P

LANES = 128
ROWS = 48
DOWN_ROWS = 120
TAPS = 3


def product(left, right, dims):
    return lax.dot_general(left, right, (dims, ((), ())), preferred_element_type=jnp.float32)


def moved(values, count):
    tokens = values.shape[0]
    turned = pltpu.roll(values, count % tokens, 0)
    row = lax.broadcasted_iota(jnp.int32, (8, values.shape[1]), 0)
    if count > 0:
        return jnp.concatenate([jnp.where(row >= count, turned[:8], 0.0), turned[8:]], 0)
    return jnp.concatenate([turned[:-8], jnp.where(row < 8 + count, turned[-8:], 0.0)], 0)


def lanes_of(c):
    return slice(c * LANES, (c + 1) * LANES)


def split_rows(out, values, lanes=slice(None)):
    start = 0
    for ref in out:
        rows = ref.shape[0]
        ref[:, lanes] = values[start : start + rows, :]
        start += rows


def slabs(length, rows, width):
    starts = range(0, length, rows)
    return [pltpu.VMEM((min(rows, length - s), width), jnp.bfloat16) for s in starts]


def whole(array):
    return pl.BlockSpec(array.shape, lambda c, *_: (0,) * len(array.shape))


def conv_kernel(place, gate, up, taps, grad, down, inputs, *refs):
    swish_out, slope_out, copies_out, one_out, down_out, *act_out = refs
    one_out[...] = taps[0:1, 0:1]
    for i in range(copies_out.shape[0]):
        copies_out[i] = inputs[...]
    for c in range(gate.shape[1] // LANES):
        lanes = lanes_of(c)
        share = product(grad[...], down[lanes, :], ((1,), (1,))).astype(jnp.bfloat16)
        split_rows(act_out, share, lanes)
        gate_float = gate[:, lanes].astype(jnp.float32)
        up_float = up[:, lanes].astype(jnp.float32)
        taps_float = taps[:, lanes].astype(jnp.float32)
        conv_out = (
            taps_float[0:1] * moved(gate_float, 2)
            + taps_float[1:2] * moved(gate_float, 1)
            + taps_float[2:3] * gate_float
        )
        sig = 0.5 * jnp.tanh(0.5 * conv_out) + 0.5
        swish = conv_out * sig
        swish_out[:, lanes] = swish.astype(jnp.bfloat16)
        slope_out[:, lanes] = (up_float * (sig + swish * (1.0 - sig))).astype(jnp.bfloat16)
        activation = (swish * up_float).astype(jnp.bfloat16)
        down_out[lanes, :] = product(activation, grad[...], ((0,), (0,))).astype(jnp.bfloat16)


def conv_cells(place, gate_saved, up_saved, conv_taps, out_grad, w_down, inputs, copies):
    tokens, hidden = gate_saved.shape
    block = w_down.shape[1]
    acts = slabs(tokens, ROWS, hidden)
    cells = pltpu.HBM((tokens, hidden), jnp.bfloat16)
    copies = pltpu.HBM((copies, *inputs.shape), inputs.dtype)
    one = jax.ShapeDtypeStruct((1, 1), jnp.bfloat16)
    down = pltpu.HBM((hidden, block), jnp.bfloat16)
    return pl.pallas_call(
        conv_kernel,
        out_shape=[cells, cells, copies, one, down] + acts,
        grid_spec=pltpu.PrefetchScalarGridSpec(
            num_scalar_prefetch=1,
            grid=(1,),
            in_specs=[
                whole(gate_saved),
                whole(up_saved),
                whole(conv_taps),
                pl.BlockSpec((tokens, block), lambda c, s: (0, s[0])),
                whole(w_down),
                whole(inputs),
            ],
            out_specs=[whole(a) for a in (cells, cells, copies, one, down)]
            + [whole(a) for a in acts],
        ),
        compiler_params=pltpu.CompilerParams(vmem_limit_bytes=32 << 20),
        name="conv_cells",
    )(place, gate_saved, up_saved, conv_taps, out_grad, w_down, inputs)


def taken(refs, counts):
    runs = []
    for count in counts:
        runs.append(refs[:count])
        refs = refs[count:]
    return *runs, refs


def grad_kernel(counts, taps, swish, slope, gate, inputs, w_gate, w_up, *refs):
    acts, (down, _, terms_out), grads_out, down_out, _ = taken(refs, counts)
    split_rows(down_out, down)
    gates, ups = [], []
    for c in range(swish.shape[1] // LANES):
        lanes = lanes_of(c)
        act_grad = jnp.concatenate([a[:, lanes] for a in acts], 0).astype(jnp.float32)
        up_part = (act_grad * swish[:, lanes].astype(jnp.float32)).astype(jnp.bfloat16)
        conv_grad = act_grad * slope[:, lanes].astype(jnp.float32)
        taps_float = taps[:, lanes].astype(jnp.float32)
        ahead_one, ahead_two = moved(conv_grad, -1), moved(conv_grad, -2)
        gate_part = (
            taps_float[0:1] * ahead_two + taps_float[1:2] * ahead_one + taps_float[2:3] * conv_grad
        ).astype(jnp.bfloat16)
        gate_float = gate[:, lanes].astype(jnp.float32)
        sums = [
            jnp.sum(ahead * gate_float, axis=0, keepdims=True)
            for ahead in (ahead_two, ahead_one, conv_grad)
        ]
        sums = jnp.concatenate(sums + [jnp.zeros((8 - TAPS, LANES), jnp.float32)], 0)
        parts = jnp.concatenate([gate_part, up_part], 1)
        grads = product(inputs[...], parts, ((1,), (0,))).astype(jnp.bfloat16)
        columns = [grads[:, :LANES], grads[:, LANES:], sums.astype(jnp.bfloat16)]
        split_rows(grads_out, jnp.concatenate(columns, 0), lanes)
        gates.append(gate_part)
        ups.append(up_part)
    weights = jnp.concatenate([w_gate[...], w_up[...]], 1)
    term = product(weights, jnp.concatenate(gates + ups, 1), ((1,), (1,)))
    terms_out[...] = term.astype(jnp.bfloat16)


def grad_cells(conv_taps, swish, slope, gate_saved, inputs, w_gate, w_up, acts, down, extra):
    tokens, hidden = swish.shape
    block = inputs.shape[0]
    grads = slabs(2 * block + 8, ROWS, hidden)
    kept = slabs(hidden, DOWN_ROWS, block)
    out = [pltpu.HBM((block, tokens), jnp.bfloat16)] + grads + kept
    counts = [len(acts), 3, len(grads), len(kept)]
    return pl.pallas_call(
        lambda *refs: grad_kernel(counts, *refs),
        out_shape=out,
        grid=(1,),
        in_specs=[whole(a) for a in (conv_taps, swish, slope, gate_saved, inputs, w_gate, w_up)]
        + [whole(a) for a in acts]
        + [whole(down), pl.BlockSpec(memory_space=pl.ANY)],
        out_specs=[whole(o) for o in out],
        compiler_params=pltpu.CompilerParams(vmem_limit_bytes=32 << 20),
        name="grad_cells",
    )(conv_taps, swish, slope, gate_saved, inputs, w_gate, w_up, *acts, down, extra)


def widen_kernel(counts, *refs):
    pairs, downs, (terms, _, input_out, gate_out, up_out, down_out, taps_out), _ = taken(refs, counts)
    block = gate_out.shape[0]
    bounds = ((gate_out, 0, block), (up_out, block, 2 * block), (taps_out, 2 * block, 2 * block + TAPS))
    start = 0
    for ref in pairs:
        values = ref[...].astype(jnp.float32)
        for out, low, high in bounds:
            first, last = max(low, start), min(high, start + ref.shape[0])
            if first < last:
                out[first - low : last - low, :] = values[first - start : last - start]
        start += ref.shape[0]
    start = 0
    for ref in downs:
        down_out[start : start + ref.shape[0], :] = ref[...].astype(jnp.float32)
        start += ref.shape[0]
    total = terms[0].astype(jnp.float32)
    for i in range(1, terms.shape[0]):
        total = total + terms[i].astype(jnp.float32)
    input_out[...] = total.astype(jnp.bfloat16)


def widened(pairs, downs, terms, extra):
    hidden = pairs[0].shape[1]
    block = downs[0].shape[1]
    grads = jax.ShapeDtypeStruct((block, hidden), jnp.float32)
    counts = [len(pairs), len(downs), 7]
    return pl.pallas_call(
        lambda *refs: widen_kernel(counts, *refs),
        out_shape=[
            jax.ShapeDtypeStruct(terms.shape[1:], jnp.bfloat16),
            grads,
            grads,
            jax.ShapeDtypeStruct((hidden, block), jnp.float32),
            jax.ShapeDtypeStruct((TAPS, hidden), jnp.float32),
        ],
        in_specs=[pl.BlockSpec(memory_space=pltpu.VMEM)] * (len(pairs) + len(downs) + 1)
        + [pl.BlockSpec(memory_space=pl.ANY)],
        compiler_params=pltpu.CompilerParams(vmem_limit_bytes=16 << 20),
        name="widened",
    )(*pairs, *downs, terms, extra)


def local(layer_input, gate_saved, up_saved, out_grad, conv_taps, w_gate, w_up, w_down):
    layer_input, gate_saved, up_saved, out_grad, conv_taps, w_gate, w_up, w_down = [
        pltpu.with_memory_space_constraint(a, pltpu.HBM)
        for a in (layer_input.T, gate_saved, up_saved, out_grad, conv_taps, w_gate, w_up, w_down)
    ]
    tp = lax.axis_size("tp")
    tokens = out_grad.shape[0]
    block = w_gate.shape[0]
    place = lax.axis_index("fs").astype(jnp.int32).reshape(1)
    swish, slope, copies, one, down, *acts = conv_cells(
        place, gate_saved, up_saved, conv_taps, out_grad, w_down, layer_input, tp
    )
    inputs = lax.all_to_all(copies, "tp", 0, 0, tiled=True).reshape(block, tokens)
    *acts, extra = lax.psum([*acts, one], "fs")
    acts = [pltpu.with_memory_space_constraint(a, pltpu.VMEM) for a in acts]
    inputs = pltpu.with_memory_space_constraint(inputs, pltpu.VMEM)
    swish, slope, down = [
        pltpu.with_memory_space_constraint(a, pltpu.HBM) for a in (swish, slope, down)
    ]
    terms, *grads = grad_cells(
        conv_taps, swish, slope, gate_saved, inputs, w_gate, w_up, acts, down, extra
    )
    terms = lax.all_to_all(terms.reshape(tp, block // tp, tokens), "tp", 0, 0, tiled=True)
    *grads, extra = lax.psum([*grads, one], "rep")
    grads = [pltpu.with_memory_space_constraint(a, pltpu.VMEM) for a in grads]
    count = len(slabs(2 * block + 8, ROWS, 1))
    input_grad, gate_grad, up_grad, down_grad, taps_grad = widened(
        grads[:count], grads[count:], terms, extra
    )
    return (input_grad.T, gate_grad, up_grad, down_grad, taps_grad)


def solution(mesh):
    placed = (
        P("rep", ("fs", "tp")),
        P("rep", "tp"),
        P("rep", "tp"),
        P("rep", None),
        P(None, "tp"),
        P("fs", "tp"),
        P("fs", "tp"),
        P("tp", "fs"),
    )
    return jax.shard_map(
        local,
        mesh=mesh,
        in_specs=placed,
        out_specs=(
            P("rep", ("fs", "tp")),
            P("fs", "tp"),
            P("fs", "tp"),
            P("tp", "fs"),
            P(None, "tp"),
        ),
        check_vma=False,
    )
```
